32 devices in a mesh: gr: 2 (over x), fs: 4 (over z), tp: 4 (over y, core).
Axes of the slice: x: 2, y: 2, z: 4, core: 2. Of those that a mesh axis runs over, the one named last changes fastest.
Arguments:
- tokens: bfloat16 [4096, 2048], P(('gr', 'fs')), may hold values from -6 to 6
- routes: int32 [4096, 2], P(('gr', 'fs')), may hold values from 0 to 3, all different within a row; in each aligned block of 512 rows (0 to 511, 512 to 1023, ...) at most 384 rows name the same one
- route_weight: float32 [4096, 2], P(('gr', 'fs')), may hold values from 0.2 to 1
- gain: float32 [2048], P(('gr', 'fs')), may hold values from 0.1 to 1.9
- w_gate: bfloat16 [4, 2048, 4096], P(None, ('gr', 'fs'), 'tp'), may hold values from -0.125 to 0.125
- w_up: bfloat16 [4, 2048, 4096], P(None, ('gr', 'fs'), 'tp'), may hold values from -0.125 to 0.125
- w_down: bfloat16 [4, 2048, 4096], P(None, ('gr', 'fs'), 'tp'), may hold values from -0.09375 to 0.09375
Outputs:
- gate_out: bfloat16 [4, 2048, 4096], P('fs', None, 'tp')
- up_out: bfloat16 [4, 2048, 4096], P('fs', None, 'tp')
- down_out: bfloat16 [4, 2048, 4096], P('fs', None, 'tp')
- mixed: bfloat16 [4096, 2048], P(('gr', 'fs'), 'tp')
The draws below stay inside these ranges and needn't reach their ends.
Inputs may be any that keep to these rules, and one draw needn't show every extreme that they name: `routes`: each row names two different experts. Among the 512 rows of one device no expert is named more than 384 times, and in every draw some device names some expert exactly 384 times.
All inputs are finite; a program needn't handle non-finite values.
Results may differ from the reference program's by a relative error of at most 0.015.
Values may be sent and summed in bfloat16 or wider, within the bound.
A program may use at most 128 MiB of HBM per device.

```python
import math
import jax
import jax.numpy as jnp
import numpy as np
from jax import lax

D = 2048
FF = 4096
EXPERTS = 4
TOK_DEV = 512
CAP = 384
TOKENS = 4096
N_GR = 2
N_FS = 4
N_TP = 4


def level_of(rng, extent, cuts, low, largest):
    def one(position, shards_of):
        heights = jax.random.uniform(jax.random.fold_in(jax.random.fold_in(rng, 6), position), (shards_of,), jnp.float32, low / len(cuts), largest / len(cuts))
        return jnp.repeat(jnp.exp(heights), extent[position] // shards_of).reshape((-1,) + (1,) * (len(extent) - position - 1))

    factor_of = one(*cuts[0])
    for cut in cuts[1:]:
        factor_of = factor_of * one(*cut)
    return factor_of


def deal_out(own_key, own, number, rows, amount, top, bound, skew):
    order = jax.random.permutation(own_key, amount)
    heavy_load, ordinary = portions_of(amount, rows * top, bound, skew, True), portions_of(amount, rows * top, bound, skew, False)
    places = jnp.arange(amount)

    def named(tallies, rotation):
        used = int((tallies > 0).sum())
        fixed = max(1, used // 4)
        passed = fixed + (places - fixed + rotation * (used - fixed)) % max(1, amount - fixed)
        return jnp.zeros((amount,), jnp.int32).at[order[jnp.where(places < fixed, places, passed)]].set(jnp.asarray(tallies, jnp.int32))

    tallies = jnp.where(number % 4 == 0, named(heavy_load, number // 4), named(ordinary, number - number // 4 - 1))
    mixed = jax.random.permutation(jax.random.fold_in(own, 3), amount)
    donor, sink = mixed[0:amount // 2 * 2:2], mixed[1:amount // 2 * 2:2]
    margin = jnp.minimum(tallies[donor] - 1, bound - tallies[sink]) // 2
    margin = jnp.where((donor == order[0]) | (sink == order[0]) | (tallies[sink] == 0), 0, jnp.maximum(margin, 0))
    passed = jax.random.randint(jax.random.fold_in(own, 4), (amount // 2,), 0, 1 << 20) % (margin + 1)
    tallies = tallies.at[donor].add(-passed).at[sink].add(passed)
    members = jnp.searchsorted(jnp.cumsum(tallies), jnp.arange(rows * top), side="right").astype(jnp.int32)
    table = members.reshape(top, rows).T
    table = table[jax.random.permutation(jax.random.fold_in(own, 1), rows)]
    rotation = jax.random.randint(jax.random.fold_in(own, 2), (rows, 1), 0, top)
    return jnp.take_along_axis(table, (jnp.arange(top)[None, :] + rotation) % top, axis=1)


def portions_of(number_of, total, most, slope, full):
    portions = [(1 << 20) // math.isqrt(standing ** slope) + 1 for standing in range(1, number_of + 1)]
    largest = most if full else min(most, max(-(-total // number_of), total * portions[0] // sum(portions)))
    least = 1 if total - largest >= number_of - 1 else 0
    counts, spare = [largest] + [least] * (number_of - 1), total - largest - least * (number_of - 1)
    while spare > 0:
        candidates = [i for i in range(1, number_of) if counts[i] < largest] or [i for i in range(1, number_of) if counts[i] < most]
        pool, budget = sum([portions[i] for i in candidates]), spare
        for i in candidates:
            extra = min(most - counts[i], max(1, budget * portions[i] // pool), spare)
            counts[i] = counts[i] + extra
            spare = spare - extra
    return np.array(counts)


def gaussian(stream_key, shape, scale, most, shards=(), kind=jnp.bfloat16):
    level = level_of(stream_key, shape, shards, -0.22, 0.18) if shards else 1.0
    drawn = jax.random.normal(stream_key, shape, jnp.float32) * scale * level
    return jnp.minimum(jnp.maximum(drawn, -most), most).astype(kind)


def setup_inputs(seed: int = 0) -> dict:
    keys = jax.random.split(jax.random.key(seed), 8)
    tokens = gaussian(keys[0], (TOKENS, D), 1.0, 6.0, ((0, 8),))
    routes_keys = jax.random.split(jax.random.fold_in(keys[1], 1), TOKENS // TOK_DEV)
    routes_turns = jax.random.permutation(jax.random.fold_in(keys[1], 3), TOKENS // TOK_DEV)
    routes = jax.vmap(lambda own, number: deal_out(jax.random.fold_in(keys[1], 2), own, number, TOK_DEV, EXPERTS, 2, CAP, 2))(routes_keys, routes_turns).reshape((TOKENS, 2))
    route_weight = jnp.clip(jnp.exp(math.log(1.0) - 1.609438 * jax.random.uniform(keys[2], (TOKENS, 2), jnp.float32) ** level_of(keys[2], (TOKENS, 2), ((0, 8),), -0.2, 0.2)), 0.2, 1.0)
    gain = jnp.clip(1.0 + 0.18 * jax.random.normal(keys[3], (D,), jnp.float32), 0.1, 1.9)
    w_gate = gaussian(keys[4], (EXPERTS, D, FF), D ** -0.5, 0.125, ((1, 8), (2, 4)))
    w_up = gaussian(keys[5], (EXPERTS, D, FF), D ** -0.5, 0.125, ((1, 8), (2, 4)))
    w_down = gaussian(keys[6], (EXPERTS, D, FF), FF ** -0.5, 0.09375, ((1, 8), (2, 4)))
    return dict(tokens=tokens, routes=routes, route_weight=route_weight, gain=gain, w_gate=w_gate, w_up=w_up, w_down=w_down)


EPSILON = 1e-05

def expert_rows(pieces):
    rows, gate_w, up_w, down_w = pieces
    gate = jnp.dot(rows, gate_w, preferred_element_type=jnp.float32)
    upper = jnp.dot(rows, up_w, preferred_element_type=jnp.float32)
    hidden = (jax.nn.silu(gate) * upper).astype(jnp.bfloat16)
    count = rows.shape[0]
    blocked = hidden.reshape(count, N_TP, FF // N_TP).astype(jnp.float32)
    down_blocks = down_w.reshape(D, N_TP, FF // N_TP).astype(jnp.float32)
    partial_value = jnp.einsum('rjf,djf->jrd', blocked, down_blocks)
    rounded = lax.optimization_barrier(partial_value.astype(jnp.bfloat16))
    return lax.optimization_barrier(jnp.sum(rounded.astype(jnp.float32), axis=0)).astype(jnp.bfloat16)

def reference(tokens, routes, route_weight, gain, w_gate, w_up, w_down):
    scaling = gain[None, :, None]
    gate_out = (w_gate.astype(jnp.float32) * scaling).astype(jnp.bfloat16)
    up_out = (w_up.astype(jnp.float32) * scaling).astype(jnp.bfloat16)
    down_out = w_down
    float_rows = tokens.astype(jnp.float32)
    normed = (float_rows * lax.rsqrt(lax.optimization_barrier(jnp.mean(float_rows * float_rows, axis=-1, keepdims=True)) + EPSILON)).astype(jnp.bfloat16)
    groups = N_GR * N_FS
    flat_ids = routes.reshape(groups, TOK_DEV * 2)
    onehot = (flat_ids[:, :, None] == jnp.arange(EXPERTS, dtype=jnp.int32)[None, None, :]).astype(jnp.int32)
    slot_rank = lax.optimization_barrier(jnp.sum((jnp.cumsum(onehot, axis=1) - onehot) * onehot, axis=-1))
    group_ids = jnp.arange(groups, dtype=jnp.int32)[:, None]
    destination = (flat_ids * (groups * CAP) + group_ids * CAP + slot_rank).reshape(-1).astype(jnp.int32)
    token_ids = (jnp.arange(TOKENS * 2, dtype=jnp.int32) // 2).astype(jnp.int32)
    source = jnp.zeros((EXPERTS * groups * CAP,), jnp.int32).at[destination].set(token_ids)
    gathered = normed[source].reshape(EXPERTS, groups * CAP, D)
    outputs = lax.map(expert_rows, (gathered, gate_out, up_out, down_out))
    flat_out = outputs.reshape(EXPERTS * groups * CAP, D)
    picked = flat_out[destination].reshape(TOKENS, 2, D).astype(jnp.float32)
    mixed = lax.optimization_barrier(jnp.sum(route_weight[:, :, None] * picked, axis=1)).astype(jnp.bfloat16)
    return (gate_out, up_out, down_out, mixed)
```

```python
import functools
import jax
import jax.numpy as jnp
from jax import lax
from jax.experimental import pallas as pl
from jax.experimental.pallas import tpu as pltpu
from jax.sharding import PartitionSpec as P

MESH = pl.DeviceIdType.MESH
VMEM_LIMIT = 66 * 1000 * 1000


def kernel(ng, nz, nt, tok_in, wt, gw, uw, dw, gout, uout, dout, mixed,
           tok, hid, part, crx, yrx, ret,
           ts, tr, fs_s, fr, ws, wr, xs, xr, cs, cr, ys, yr, rs, rr):
    g, z, t = lax.axis_index("gr"), lax.axis_index("fs"), lax.axis_index("tp")
    core, y = lax.rem(t, 2), lax.div(t, 2)
    rows, quarter = tok_in.shape[1], tok_in.shape[2]
    chunk, width = gw.shape[1], gw.shape[2]
    chunks = ng * nz
    per_owner = chunks // nt
    srcs = (gw, uw, dw)
    outs = (gout, uout, dout)
    ks = sorted(range(1, nz), key=lambda k: min(k, nz - k))

    def to(k):
        return lax.rem(z + k, nz)

    def frm(k):
        return lax.rem(z + nz - k, nz)

    def rdma(src, dst, ss, rsem, dev):
        return pltpu.make_async_remote_copy(
            src_ref=src, dst_ref=dst, send_sem=ss, recv_sem=rsem, device_id=dev, device_id_type=MESH
        )

    def rows_of(m, group, zs):
        return outs[m].at[pl.ds(pl.multiple_of((group * nz + zs) * chunk, chunk), chunk), :]

    barrier = pltpu.get_barrier_semaphore()
    for k in range(1, nz):
        pl.semaphore_signal(barrier, inc=1, device_id={"fs": to(k)}, device_id_type=MESH)
    for j in range(1, nt):
        pl.semaphore_signal(barrier, inc=1, device_id={"tp": lax.rem(t + j, nt)}, device_id_type=MESH)
    pl.semaphore_signal(barrier, inc=1, device_id={"gr": 1 - g}, device_id_type=MESH)
    pl.semaphore_wait(barrier, nz + nt - 1)

    sends = []

    def z_send(m, k):
        c = rdma(srcs[m].at[to(k)], rows_of(m, g, z), ws.at[m, k], wr.at[m, k], {"fs": to(k)})
        c.start()
        sends.append(c)

    def x_send(m, k, src):
        c = rdma(src, rows_of(m, g, frm(k)), xs.at[m, k], xr.at[m, k], {"gr": 1 - g})
        c.start()
        sends.append(c)

    def z_take(m, k):
        ref = rows_of(m, g, frm(k))
        rdma(ref, ref, ws.at[m, k], wr.at[m, k], {"fs": to(k)}).wait_recv()
        x_send(m, k, ref)

    def x_take(m, k):
        ref = rows_of(m, 1 - g, frm(k))
        rdma(ref, ref, xs.at[m, k], xr.at[m, k], {"gr": 1 - g}).wait_recv()

    for m in range(3):
        x_send(m, 0, srcs[m].at[z])
    for k in ks:
        c = rdma(tok_in.at[t], tok.at[t, z], ts.at[k], tr.at[k], {"fs": to(k)})
        c.start()
        sends.append(c)
    for m in range(2):
        for k in ks:
            z_send(m, k)
    for m in range(3):
        outs[m][pl.ds(pl.multiple_of((g * nz + z) * chunk, chunk), chunk), :] = srcs[m][z]
    for q in range(nt):
        tok[q, z] = tok_in[q]
    for k in ks:
        ref = tok.at[t, frm(k)]
        rdma(ref, ref, ts.at[k], tr.at[k], {"fs": to(k)}).wait_recv()
        for j in range(1, nt):
            c = rdma(ref, ref, fs_s.at[j, k], fr.at[j, k], {"tp": lax.rem(t + j, nt)})
            c.start()
            sends.append(c)
    for k in ks:
        z_send(2, k)
    for m in range(2):
        for k in ks:
            z_take(m, k)
    for k in ks:
        for j in range(1, nt):
            ref = tok.at[lax.rem(t + nt - j, nt), frm(k)]
            rdma(ref, ref, fs_s.at[j, k], fr.at[j, k], {"tp": lax.rem(t + j, nt)}).wait_recv()
    for m in range(2):
        for k in [0] + ks:
            x_take(m, k)

    tile = 256
    tiles = width // tile

    def hidden(lo, hi):
        @pl.loop(lo * tiles, hi * tiles)
        def _(i):
            b = i // tiles
            cols = pl.ds(pl.multiple_of((i % tiles) * tile, tile), tile)
            gate = jnp.zeros((rows, tile), jnp.float32)
            upper = jnp.zeros((rows, tile), jnp.float32)
            for q in range(nt):
                a = tok[q, b]
                gate += jnp.dot(a, gout[q * quarter:(q + 1) * quarter, cols], preferred_element_type=jnp.float32)
                upper += jnp.dot(a, uout[q * quarter:(q + 1) * quarter, cols], preferred_element_type=jnp.float32)
            hid[b, :, cols] = (gate / (1.0 + jnp.exp(-gate)) * upper).astype(jnp.bfloat16)

    cuts = [nz * (i + 1) // nz for i in range(nz)]
    late = list(ks)
    done = 0
    for i, hi in enumerate(cuts):
        hidden(done, hi)
        done = hi
        if i >= 1 and len(late) > 1:
            z_take(2, late.pop(0))

    def ids(c):
        owner = c // per_owner
        return owner, lax.rem(owner, 2), lax.div(owner, 2), lax.rem(c, per_owner)

    finals = []

    def stage_a(i, c):
        mine = pl.ds(pl.multiple_of(c * chunk, chunk), chunk)

        @pl.loop(0, nz)
        def _(b):
            part[c, b] = lax.dot_general(
                hid[b], dout[mine, :], (((1,), (1,)), ((), ())), preferred_element_type=jnp.float32
            ).astype(jnp.bfloat16)

        owner, par, yo, cc = ids(c)
        give = rdma(part.at[c], crx.at[yo * per_owner + cc], cs.at[i], cr.at[i], {"tp": y * 2 + 1 - core})

        @pl.when(par != core)
        def _():
            give.start()
        finals.append((par != core, give))

    def stage_b(i, c):
        owner, par, yo, cc = ids(c)
        up = rdma(part.at[c], yrx.at[cc], ys.at[i], yr.at[i], {"tp": yo * 2 + core})
        away = jnp.logical_and(par == core, yo != y)

        @pl.when(par == core)
        def _():
            slot = crx.at[yo * per_owner + cc]
            rdma(slot, slot, cs.at[i], cr.at[i], {"tp": y * 2 + 1 - core}).wait_recv()

            @pl.loop(0, nz)
            def _(b):
                part[c, b] = (
                    part[c, b].astype(jnp.float32) + crx[yo * per_owner + cc, b].astype(jnp.float32)
                ).astype(jnp.bfloat16)

        @pl.when(away)
        def _():
            up.start()
        finals.append((away, up))

    def stage_c(i, c):
        owner, par, yo, cc = ids(c)
        home = [
            rdma(part.at[c, to(k)], ret.at[z, cc], rs.at[k, cc], rr.at[k, cc], {"fs": to(k)}) for k in ks
        ]

        @pl.when(owner == t)
        def _():
            slot = yrx.at[cc]
            rdma(slot, slot, ys.at[i], yr.at[i], {"tp": (1 - y) * 2 + core}).wait_recv()

            @pl.loop(0, nz)
            def _(b):
                part[c, b] = (
                    part[c, b].astype(jnp.float32) + yrx[cc, b].astype(jnp.float32)
                ).astype(jnp.bfloat16)
            for h in home:
                h.start()
            ret[z, cc] = part[c, z]
        for h in home:
            finals.append((owner == t, h))

    order = [(0, 0), (1, 0)] + [(0, k) for k in ks] + [(1, k) for k in ks]
    seq = [((g if side == 0 else 1 - g) * nz + frm(k), side, k) for side, k in order]
    n = len(seq)
    for i in range(n + 2):
        if i < n:
            c, side, k = seq[i]
            if side == 1:
                x_take(2, k)
            elif k in late:
                z_take(2, k)
                late.remove(k)
            stage_a(i, c)
        if 0 <= i - 1 < n:
            stage_b(i - 1, seq[i - 1][0])
        if 0 <= i - 2 < n:
            stage_c(i - 2, seq[i - 2][0])

    for k in ks:
        for cc in range(per_owner):
            ref = ret.at[frm(k), cc]
            rdma(ref, ref, rs.at[k, cc], rr.at[k, cc], {"fs": to(k)}).wait_recv()
    for cc in range(per_owner):
        total = wt[:, 0:1] * ret[0, cc].astype(jnp.float32)
        for e in range(1, nz):
            total += wt[:, e:e + 1] * ret[e, cc].astype(jnp.float32)
        mixed[:, cc * chunk:(cc + 1) * chunk] = total.astype(jnp.bfloat16)
    for c in sends:
        c.wait_send()
    for flag, c in finals:
        @pl.when(flag)
        def _(c=c):
            c.wait_send()


def fused(ng, nz, nt, tokens, routes, route_weight, gain, w_gate, w_up, w_down):
    scaling = gain[None, :, None]
    gate_local = (w_gate * scaling).astype(jnp.bfloat16)
    up_local = (w_up * scaling).astype(jnp.bfloat16)
    rows, d = tokens.shape
    quarter = d // nt
    experts, chunk, width = w_gate.shape
    chunks = ng * nz
    per_owner = chunks // nt
    float_rows = tokens.astype(jnp.float32)
    normed = (
        float_rows * lax.rsqrt(jnp.mean(float_rows * float_rows, axis=-1, keepdims=True) + EPSILON)
    ).astype(jnp.bfloat16)
    normed = normed.reshape(rows, nt, quarter).transpose(1, 0, 2)
    ids = jnp.arange(experts, dtype=jnp.int32)
    wt = jnp.sum(jnp.where(routes[:, :, None] == ids, route_weight[:, :, None], 0.0), axis=1)
    bf = jnp.bfloat16
    dma = pltpu.SemaphoreType.DMA
    full = jax.ShapeDtypeStruct((d, width), bf)
    vmem = pl.BlockSpec(memory_space=pltpu.VMEM)
    outs = pl.pallas_call(
        functools.partial(kernel, ng, nz, nt),
        out_shape=(full, full, full, jax.ShapeDtypeStruct((rows, quarter), bf)),
        in_specs=[vmem] * 5,
        out_specs=(vmem,) * 4,
        scratch_shapes=[
            pltpu.VMEM((nt, nz, rows, quarter), bf),
            pltpu.VMEM((nz, rows, width), bf),
            pltpu.VMEM((chunks, nz, rows, chunk), bf),
            pltpu.VMEM((chunks // 2, nz, rows, chunk), bf),
            pltpu.VMEM((per_owner, nz, rows, chunk), bf),
            pltpu.VMEM((nz, per_owner, rows, chunk), bf),
            dma((nz,)), dma((nz,)),
            dma((nt, nz)), dma((nt, nz)),
            dma((3, nz)), dma((3, nz)),
            dma((3, nz)), dma((3, nz)),
            dma((chunks,)), dma((chunks,)),
            dma((chunks,)), dma((chunks,)),
            dma((nz, per_owner)), dma((nz, per_owner)),
        ],
        compiler_params=pltpu.CompilerParams(
            collective_id=0, has_side_effects=True, vmem_limit_bytes=VMEM_LIMIT
        ),
    )(normed, wt, gate_local, up_local, w_down)
    gate_out, up_out, down_out, mixed = outs
    return (gate_out[None], up_out[None], down_out[None], mixed)

EXP_DEV = 1


EPSILON = 1e-05


def body(tokens, routes, route_weight, gain, w_gate, w_up, w_down):
    scaling = gain[None, :, None]
    gate_local = (w_gate * scaling).astype(jnp.bfloat16)
    up_local = (w_up * scaling).astype(jnp.bfloat16)
    gate_mine, up_mine, down_mine = (
        lax.all_to_all(gate_local, "fs", split_axis=0, concat_axis=1, tiled=True),
        lax.all_to_all(up_local, "fs", split_axis=0, concat_axis=1, tiled=True),
        lax.all_to_all(w_down, "fs", split_axis=0, concat_axis=1, tiled=True),
    )
    gate_out, up_out, down_out = (
        lax.all_gather(gate_mine, "gr", axis=1, tiled=True),
        lax.all_gather(up_mine, "gr", axis=1, tiled=True),
        lax.all_gather(down_mine, "gr", axis=1, tiled=True),
    )
    fs_count = lax.axis_size("fs")
    experts = EXP_DEV * fs_count
    tok_rows = tokens.shape[0]
    capacity = 3 * tok_rows // experts
    float_rows = tokens.astype(jnp.float32)
    normed = (
        float_rows * lax.rsqrt(jnp.mean(float_rows * float_rows, axis=-1, keepdims=True) + EPSILON)
    ).astype(jnp.bfloat16)
    flat_ids = routes.reshape(-1)
    onehot = (flat_ids[:, None] == jnp.arange(experts, dtype=jnp.int32)[None, :]).astype(jnp.int32)
    slot_rank = jnp.sum((jnp.cumsum(onehot, axis=0) - onehot) * onehot, axis=-1)
    destination = (flat_ids * capacity + slot_rank).reshape(tok_rows, 2)
    slot_ids = jnp.arange(experts * capacity, dtype=jnp.int32)
    hits = slot_ids[:, None, None] == destination[None, :, :]
    dispatch = jnp.any(hits, axis=-1).astype(jnp.bfloat16)
    outgoing = jnp.dot(dispatch, normed, preferred_element_type=jnp.float32).astype(jnp.bfloat16)
    outgoing = outgoing.reshape(fs_count, EXP_DEV, capacity, tokens.shape[1])
    arrived = lax.all_to_all(outgoing, "fs", split_axis=0, concat_axis=0, tiled=True)
    gate = jnp.einsum("sjnd,jdf->sjnf", arrived, gate_out, preferred_element_type=jnp.float32)
    upper = jnp.einsum("sjnd,jdf->sjnf", arrived, up_out, preferred_element_type=jnp.float32)
    hidden = (jax.nn.silu(gate) * upper).astype(jnp.bfloat16)
    partial_value = jnp.einsum(
        "sjnf,jdf->sjnd", hidden, down_out, preferred_element_type=jnp.float32
    )
    rounded = lax.optimization_barrier(partial_value.astype(jnp.bfloat16))
    summed = lax.psum_scatter(
        rounded.astype(jnp.float32).astype(jnp.bfloat16), "tp", scatter_dimension=3, tiled=True
    )
    back_home = lax.all_to_all(summed, "fs", split_axis=0, concat_axis=0, tiled=True)
    features = back_home.shape[-1]
    flat_back = back_home.reshape(experts * capacity, features).astype(jnp.float32)
    first = jnp.where(slot_ids[None, :] == destination[:, 0:1], route_weight[:, 0:1], 0.0)
    second = jnp.where(slot_ids[None, :] == destination[:, 1:2], route_weight[:, 1:2], 0.0)
    combine_map = first + second
    mixed = jnp.dot(
        combine_map, flat_back, precision=lax.Precision.HIGHEST, preferred_element_type=jnp.float32
    ).astype(jnp.bfloat16)
    return (gate_out, up_out, down_out, mixed)


def solution(mesh):
    in_specs = (
        P(("gr", "fs"), None),
        P(("gr", "fs"), None),
        P(("gr", "fs"), None),
        P(("gr", "fs")),
        P(None, ("gr", "fs"), "tp"),
        P(None, ("gr", "fs"), "tp"),
        P(None, ("gr", "fs"), "tp"),
    )
    out_specs = (
        P("fs", None, "tp"),
        P("fs", None, "tp"),
        P("fs", None, "tp"),
        P(("gr", "fs"), "tp"),
    )
    ng, nz, nt = mesh.shape["gr"], mesh.shape["fs"], mesh.shape["tp"]
    small = ng == 2 and nt == 4 and nz <= 4
    work = functools.partial(fused, ng, nz, nt) if small else body
    return jax.shard_map(work, mesh=mesh, in_specs=in_specs, out_specs=out_specs, check_vma=False)
```

```python
import functools
import jax
import jax.numpy as jnp
from jax import lax
from jax.experimental import pallas as pl
from jax.experimental.pallas import tpu as pltpu
from jax.sharding import PartitionSpec as P

MESH = pl.DeviceIdType.MESH
VMEM_LIMIT = 66 * 1000 * 1000
EPSILON = 1e-05


def kernel(ng, nz, nt, tok_in, wt, gw, uw, dw, gout, uout, dout, mixed,
           tok, hid, part, crx, yrx, ret,
           ts, tr, fs_s, fr, own, ws, wr, xs, xr, cs, cr, ys, yr, rs, rr):
    g, z, t = lax.axis_index("gr"), lax.axis_index("fs"), lax.axis_index("tp")
    core, y = lax.rem(t, 2), lax.div(t, 2)
    rows, quarter = tok_in.shape[0], tok_in.shape[1] // nt
    chunk, width = gw.shape[1], gw.shape[2]
    chunks = ng * nz
    per_owner = chunks // nt
    srcs = (gw, uw, dw)
    outs = (gout, uout, dout)
    ks = sorted(range(1, nz), key=lambda k: min(k, nz - k))

    def to(k):
        return lax.rem(z + k, nz)

    def frm(k):
        return lax.rem(z + nz - k, nz)

    def rdma(src, dst, ss, rsem, dev):
        return pltpu.make_async_remote_copy(
            src_ref=src, dst_ref=dst, send_sem=ss, recv_sem=rsem, device_id=dev, device_id_type=MESH
        )

    def rows_of(m, group, zs):
        return outs[m].at[pl.ds(pl.multiple_of((group * nz + zs) * chunk, chunk), chunk), :]

    barrier = pltpu.get_barrier_semaphore()
    for k in range(1, nz):
        pl.semaphore_signal(barrier, inc=1, device_id={"fs": to(k)}, device_id_type=MESH)
    for j in range(1, nt):
        pl.semaphore_signal(barrier, inc=1, device_id={"tp": lax.rem(t + j, nt)}, device_id_type=MESH)
    pl.semaphore_signal(barrier, inc=1, device_id={"gr": 1 - g}, device_id_type=MESH)
    pl.semaphore_wait(barrier, nz + nt - 1)

    sends = []

    def z_send(m, k):
        c = rdma(srcs[m].at[to(k)], rows_of(m, g, z), ws.at[m, k], wr.at[m, k], {"fs": to(k)})
        c.start()
        sends.append(c)

    def x_send(m, k, src):
        c = rdma(src, rows_of(m, g, frm(k)), xs.at[m, k], xr.at[m, k], {"gr": 1 - g})
        c.start()
        sends.append(c)

    def z_take(m, k):
        ref = rows_of(m, g, frm(k))
        rdma(ref, ref, ws.at[m, k], wr.at[m, k], {"fs": to(k)}).wait_recv()
        x_send(m, k, ref)

    def x_take(m, k):
        ref = rows_of(m, 1 - g, frm(k))
        rdma(ref, ref, xs.at[m, k], xr.at[m, k], {"gr": 1 - g}).wait_recv()

    x_send(0, 0, gw.at[z])
    for k in ks:
        z_send(0, k)
    x_send(1, 0, uw.at[z])
    x_send(2, 0, dw.at[z])
    own_rows = pl.ds(pl.multiple_of((g * nz + z) * chunk, chunk), chunk)
    own_down = pltpu.make_async_copy(dw.at[z], dout.at[own_rows, :], own)
    own_down.start()

    step = 64

    @pl.loop(0, rows // step)
    def _(i):
        at = pl.ds(pl.multiple_of(i * step, step), step)
        x = tok_in[at, :].astype(jnp.float32)
        scale = lax.rsqrt(jnp.mean(x * x, axis=-1, keepdims=True) + EPSILON)
        x = (x * scale).astype(jnp.bfloat16)
        for q in range(nt):
            tok[q, z, at, :] = x[:, q * quarter:(q + 1) * quarter]

    for m in range(2):
        outs[m][own_rows, :] = srcs[m][z]

    guarded = []

    def guard(flag, c):
        @pl.when(flag)
        def _():
            c.start()
        guarded.append((flag, c))

    def hop(way, h, src):
        nxt = lax.rem(z + way + nz, nz)
        ref = tok.at[t, src]
        return rdma(ref, ref, ts.at[(way + 1) // 2, h], tr.at[src], {"fs": nxt})

    right, left = z + 1 < nz, z >= 1
    guard(right, hop(1, 0, z))
    guard(left, hop(-1, 0, z))
    z_send(1, ks[0])
    for k in ks:
        z_take(0, k)
    mate, over = y * 2 + 1 - core, (1 - y) * 2 + core
    for h in range(1, nz):
        for way in (1, -1):
            src = lax.rem(z - way * h + nz, nz)
            valid = z >= h if way == 1 else z + h < nz
            more = right if way == 1 else left
            ref = tok.at[t, src]

            @pl.when(valid)
            def _(ref=ref, src=src):
                rdma(ref, ref, ts.at[0, 0], tr.at[src], {"fs": lax.rem(z + 1, nz)}).wait_recv()
            guard(jnp.logical_and(valid, more), hop(way, h, src))
            guard(valid, rdma(ref, ref, fs_s.at[1, src], fr.at[1, src], {"tp": over}))
            guard(valid, rdma(ref, ref, fs_s.at[0, src], fr.at[0, src], {"tp": mate}))
        if h < len(ks):
            z_send(1, ks[h])
    for k in ks:
        z_send(2, k)
    z_take(1, ks[0])
    for k in ks:
        src = frm(k)
        ref = tok.at[over, src]
        rdma(ref, ref, fs_s.at[1, src], fr.at[1, src], {"tp": over}).wait_recv()
        c = rdma(ref, ref, fs_s.at[2, src], fr.at[2, src], {"tp": mate})
        c.start()
        sends.append(c)
    for k in ks[1:]:
        z_take(1, k)
    for k in ks:
        src = frm(k)
        for lane, who in ((0, mate), (2, (1 - y) * 2 + 1 - core)):
            ref = tok.at[who, src]
            rdma(ref, ref, fs_s.at[lane, src], fr.at[lane, src], {"tp": mate}).wait_recv()
    for m in range(2):
        for k in [0] + ks:
            x_take(m, k)

    tile = 256
    tiles = width // tile

    def hidden(lo, hi):
        @pl.loop(lo * tiles, hi * tiles)
        def _(i):
            b = i // tiles
            cols = pl.ds(pl.multiple_of((i % tiles) * tile, tile), tile)
            gate = jnp.zeros((rows, tile), jnp.float32)
            upper = jnp.zeros((rows, tile), jnp.float32)
            for q in range(nt):
                a = tok[q, b]
                gate += jnp.dot(a, gout[q * quarter:(q + 1) * quarter, cols], preferred_element_type=jnp.float32)
                upper += jnp.dot(a, uout[q * quarter:(q + 1) * quarter, cols], preferred_element_type=jnp.float32)
            hid[b, :, cols] = (gate / (1.0 + jnp.exp(-gate)) * upper).astype(jnp.bfloat16)

    cuts = [nz * (i + 1) // nz for i in range(nz)]
    late = list(ks)
    done = 0
    for i, hi in enumerate(cuts):
        hidden(done, hi)
        done = hi
        if i >= 1 and late:
            z_take(2, late.pop(0))

    def ids(c):
        owner = c // per_owner
        return owner, lax.rem(owner, 2), lax.div(owner, 2), lax.rem(c, per_owner)

    own_down.wait()
    finals = guarded

    def stage_a(i, c):
        mine = pl.ds(pl.multiple_of(c * chunk, chunk), chunk)

        @pl.loop(0, nz)
        def _(b):
            part[c, b] = lax.dot_general(
                hid[b], dout[mine, :], (((1,), (1,)), ((), ())), preferred_element_type=jnp.float32
            ).astype(jnp.bfloat16)

        owner, par, yo, cc = ids(c)
        give = rdma(part.at[c], crx.at[yo * per_owner + cc], cs.at[i], cr.at[i], {"tp": y * 2 + 1 - core})

        @pl.when(par != core)
        def _():
            give.start()
        finals.append((par != core, give))

    def stage_b(i, c):
        owner, par, yo, cc = ids(c)
        up = rdma(part.at[c], yrx.at[cc], ys.at[i], yr.at[i], {"tp": yo * 2 + core})
        away = jnp.logical_and(par == core, yo != y)

        @pl.when(par == core)
        def _():
            slot = crx.at[yo * per_owner + cc]
            rdma(slot, slot, cs.at[i], cr.at[i], {"tp": y * 2 + 1 - core}).wait_recv()

            @pl.loop(0, nz)
            def _(b):
                part[c, b] = (
                    part[c, b].astype(jnp.float32) + crx[yo * per_owner + cc, b].astype(jnp.float32)
                ).astype(jnp.bfloat16)

        @pl.when(away)
        def _():
            up.start()
        finals.append((away, up))

    def stage_c(i, c):
        owner, par, yo, cc = ids(c)
        home = [
            rdma(part.at[c, to(k)], ret.at[z, cc], rs.at[k, cc], rr.at[k, cc], {"fs": to(k)}) for k in ks
        ]

        @pl.when(owner == t)
        def _():
            slot = yrx.at[cc]
            rdma(slot, slot, ys.at[i], yr.at[i], {"tp": (1 - y) * 2 + core}).wait_recv()

            @pl.loop(0, nz)
            def _(b):
                part[c, b] = (
                    part[c, b].astype(jnp.float32) + yrx[cc, b].astype(jnp.float32)
                ).astype(jnp.bfloat16)
            for h in home:
                h.start()
            ret[z, cc] = part[c, z]
        for h in home:
            finals.append((owner == t, h))

    order = [(side, k) for k in [0] + ks for side in (0, 1)]
    lag = 4
    seq = [((g if side == 0 else 1 - g) * nz + frm(k), side, k) for side, k in order]
    n = len(seq)
    for i in range(n + lag):
        if i < n:
            c, side, k = seq[i]
            if side == 1:
                x_take(2, k)
            stage_a(i, c)
        if 0 <= i - 1 < n:
            stage_b(i - 1, seq[i - 1][0])
        if 0 <= i - lag < n:
            stage_c(i - lag, seq[i - lag][0])

    for k in ks:
        for cc in range(per_owner):
            ref = ret.at[frm(k), cc]
            rdma(ref, ref, rs.at[k, cc], rr.at[k, cc], {"fs": to(k)}).wait_recv()
    for cc in range(per_owner):
        total = wt[:, 0:1] * ret[0, cc].astype(jnp.float32)
        for e in range(1, nz):
            total += wt[:, e:e + 1] * ret[e, cc].astype(jnp.float32)
        mixed[:, cc * chunk:(cc + 1) * chunk] = total.astype(jnp.bfloat16)
    for c in sends:
        c.wait_send()
    for flag, c in finals:
        @pl.when(flag)
        def _(c=c):
            c.wait_send()


def fused(ng, nz, nt, tokens, routes, route_weight, gain, w_gate, w_up, w_down):
    scaling = gain[None, :, None]
    gate_local = (w_gate * scaling).astype(jnp.bfloat16)
    up_local = (w_up * scaling).astype(jnp.bfloat16)
    rows, d = tokens.shape
    quarter = d // nt
    experts, chunk, width = w_gate.shape
    chunks = ng * nz
    per_owner = chunks // nt
    ids = jnp.arange(experts, dtype=jnp.int32)
    wt = jnp.sum(jnp.where(routes[:, :, None] == ids, route_weight[:, :, None], 0.0), axis=1)
    bf = jnp.bfloat16
    dma = pltpu.SemaphoreType.DMA
    full = jax.ShapeDtypeStruct((d, width), bf)
    vmem = pl.BlockSpec(memory_space=pltpu.VMEM)
    outs = pl.pallas_call(
        functools.partial(kernel, ng, nz, nt),
        out_shape=(full, full, full, jax.ShapeDtypeStruct((rows, quarter), bf)),
        in_specs=[vmem] * 4 + [pl.BlockSpec(memory_space=pl.ANY)],
        out_specs=(vmem,) * 4,
        scratch_shapes=[
            pltpu.VMEM((nt, nz, rows, quarter), bf),
            pltpu.VMEM((nz, rows, width), bf),
            pltpu.VMEM((chunks, nz, rows, chunk), bf),
            pltpu.VMEM((chunks // 2, nz, rows, chunk), bf),
            pltpu.VMEM((per_owner, nz, rows, chunk), bf),
            pltpu.VMEM((nz, per_owner, rows, chunk), bf),
            dma((2, nz)), dma((nz,)),
            dma((3, nz)), dma((3, nz)), dma,
            dma((3, nz)), dma((3, nz)),
            dma((3, nz)), dma((3, nz)),
            dma((chunks,)), dma((chunks,)),
            dma((chunks,)), dma((chunks,)),
            dma((nz, per_owner)), dma((nz, per_owner)),
        ],
        compiler_params=pltpu.CompilerParams(
            collective_id=0, has_side_effects=True, vmem_limit_bytes=VMEM_LIMIT
        ),
    )(tokens, wt, gate_local, up_local, w_down)
    gate_out, up_out, down_out, mixed = outs
    return (gate_out[None], up_out[None], down_out[None], mixed)

EXP_DEV = 1


def body(tokens, routes, route_weight, gain, w_gate, w_up, w_down):
    scaling = gain[None, :, None]
    gate_local = (w_gate * scaling).astype(jnp.bfloat16)
    up_local = (w_up * scaling).astype(jnp.bfloat16)
    gate_mine, up_mine, down_mine = (
        lax.all_to_all(gate_local, "fs", split_axis=0, concat_axis=1, tiled=True),
        lax.all_to_all(up_local, "fs", split_axis=0, concat_axis=1, tiled=True),
        lax.all_to_all(w_down, "fs", split_axis=0, concat_axis=1, tiled=True),
    )
    gate_out, up_out, down_out = (
        lax.all_gather(gate_mine, "gr", axis=1, tiled=True),
        lax.all_gather(up_mine, "gr", axis=1, tiled=True),
        lax.all_gather(down_mine, "gr", axis=1, tiled=True),
    )
    fs_count = lax.axis_size("fs")
    experts = EXP_DEV * fs_count
    tok_rows = tokens.shape[0]
    capacity = 3 * tok_rows // experts
    float_rows = tokens.astype(jnp.float32)
    normed = (
        float_rows * lax.rsqrt(jnp.mean(float_rows * float_rows, axis=-1, keepdims=True) + EPSILON)
    ).astype(jnp.bfloat16)
    flat_ids = routes.reshape(-1)
    onehot = (flat_ids[:, None] == jnp.arange(experts, dtype=jnp.int32)[None, :]).astype(jnp.int32)
    slot_rank = jnp.sum((jnp.cumsum(onehot, axis=0) - onehot) * onehot, axis=-1)
    destination = (flat_ids * capacity + slot_rank).reshape(tok_rows, 2)
    slot_ids = jnp.arange(experts * capacity, dtype=jnp.int32)
    hits = slot_ids[:, None, None] == destination[None, :, :]
    dispatch = jnp.any(hits, axis=-1).astype(jnp.bfloat16)
    outgoing = jnp.dot(dispatch, normed, preferred_element_type=jnp.float32).astype(jnp.bfloat16)
    outgoing = outgoing.reshape(fs_count, EXP_DEV, capacity, tokens.shape[1])
    arrived = lax.all_to_all(outgoing, "fs", split_axis=0, concat_axis=0, tiled=True)
    gate = jnp.einsum("sjnd,jdf->sjnf", arrived, gate_out, preferred_element_type=jnp.float32)
    upper = jnp.einsum("sjnd,jdf->sjnf", arrived, up_out, preferred_element_type=jnp.float32)
    hidden = (jax.nn.silu(gate) * upper).astype(jnp.bfloat16)
    partial_value = jnp.einsum(
        "sjnf,jdf->sjnd", hidden, down_out, preferred_element_type=jnp.float32
    )
    rounded = lax.optimization_barrier(partial_value.astype(jnp.bfloat16))
    summed = lax.psum_scatter(
        rounded.astype(jnp.float32).astype(jnp.bfloat16), "tp", scatter_dimension=3, tiled=True
    )
    back_home = lax.all_to_all(summed, "fs", split_axis=0, concat_axis=0, tiled=True)
    features = back_home.shape[-1]
    flat_back = back_home.reshape(experts * capacity, features).astype(jnp.float32)
    first = jnp.where(slot_ids[None, :] == destination[:, 0:1], route_weight[:, 0:1], 0.0)
    second = jnp.where(slot_ids[None, :] == destination[:, 1:2], route_weight[:, 1:2], 0.0)
    combine_map = first + second
    mixed = jnp.dot(
        combine_map, flat_back, precision=lax.Precision.HIGHEST, preferred_element_type=jnp.float32
    ).astype(jnp.bfloat16)
    return (gate_out, up_out, down_out, mixed)


def solution(mesh):
    in_specs = (
        P(("gr", "fs"), None),
        P(("gr", "fs"), None),
        P(("gr", "fs"), None),
        P(("gr", "fs")),
        P(None, ("gr", "fs"), "tp"),
        P(None, ("gr", "fs"), "tp"),
        P(None, ("gr", "fs"), "tp"),
    )
    out_specs = (
        P("fs", None, "tp"),
        P("fs", None, "tp"),
        P("fs", None, "tp"),
        P(("gr", "fs"), "tp"),
    )
    ng, nz, nt = mesh.shape["gr"], mesh.shape["fs"], mesh.shape["tp"]
    small = ng == 2 and nt == 4 and nz <= 4
    work = functools.partial(fused, ng, nz, nt) if small else body
    return jax.shard_map(work, mesh=mesh, in_specs=in_specs, out_specs=out_specs, check_vma=False)
```
